32 devices in a mesh: ep: 8 (over z, x), tp: 4 (over y, core).
Axes of the slice: x: 2, y: 2, z: 4, core: 2. Of those that a mesh axis runs over, the one named last changes fastest.
Arguments:
- query_in: bfloat16 [4096, 2048], P('ep', 'tp'), may hold values from -6 to 6
- key_in: bfloat16 [4096, 2048], P('ep', 'tp'), may hold values from -6 to 6
- value_in: bfloat16 [4096, 2048], P('ep', 'tp'), may hold values from -6 to 6
- gate_in: bfloat16 [4096, 2048], P('ep', 'tp'), may hold values from -6 to 6
- decay_rate: float32 [16], P('tp'), may hold values from 0 to 0.04
- head_gain: float32 [2048], P('tp'), may hold values from 0.1 to 1.9
- output_weight: bfloat16 [2048, 2048], P('tp'), may hold values from -0.125 to 0.125
- token_rows: bfloat16 [1536, 2048], P('ep'), may hold values from -100 to 100
- token_gain: float32 [2048], replicated, may hold values from 0.1 to 1.9
- route_ids: int32 [1536, 2], P('ep'), may hold values from 0 to 7, all different within a row; in each aligned block of 192 rows (0 to 191, 192 to 383, ...) at most 96 rows name the same one
- route_weights: float32 [1536, 2], P('ep'), may hold values from 0.25 to 2.5
- expert_gate: bfloat16 [8, 2048, 4096], P('ep', None, 'tp'), may hold values from -0.125 to 0.125
- expert_up: bfloat16 [8, 2048, 4096], P('ep', None, 'tp'), may hold values from -0.125 to 0.125
- expert_down: bfloat16 [8, 4096, 2048], P('ep', None, 'tp'), may hold values from -0.09375 to 0.09375
Outputs:
- retained_out: bfloat16 [4096, 2048], P(('ep', 'tp'))
- expert_out: bfloat16 [1536, 2048], P('ep', 'tp')
The draws below stay inside these ranges and needn't reach their ends.
Inputs may be any that keep to these rules, and one draw needn't show every extreme that they name: `route_ids`: each row names 2 different experts. In each aligned block of 192 rows (the rows of one index of ep) no expert is named by more than 96 rows, a bound that some block reaches.
All inputs are finite; a program needn't handle non-finite values.
Results may differ from the reference program's by a relative error of at most 0.019.
Values may be sent and summed in bfloat16 or wider, within the bound.
A program may use at most 64 MiB of HBM per device.

```python
import math
import jax
import jax.numpy as jnp
import numpy as np
from jax import lax

D = 2048
HEADS = 16
DK = 128
DV = 128
FF = 4096
TOP = 2
TOK_MIX = 512
TOK_MOE = 192
EXPERTS = 8
SEQ_MIX = 4096
TOKENS_MOE = 1536
CAP = 96
N_EP = 8
N_TP = 4


def draw_decay_rate(key, part):
    subkeys = jax.random.split(jax.random.fold_in(key, 11), 3)
    fast_share = 0.5
    is_fast = jax.random.uniform(subkeys[0], (HEADS,)) < fast_share
    fast_rate = jnp.exp(jax.random.uniform(subkeys[1], (HEADS,), minval=jnp.log(0.01), maxval=jnp.log(1.0 / 30.0)))
    slow_rate = jnp.exp(jax.random.uniform(subkeys[2], (HEADS,), minval=jnp.log(0.1 / SEQ_MIX), maxval=jnp.log(1.5 / SEQ_MIX)))
    return jnp.where(is_fast, fast_rate, slow_rate).astype(jnp.float32)


def draw_value_in(key, part):
    subkeys = jax.random.split(jax.random.fold_in(key, 37), 2)
    row_scale = jnp.exp(jax.random.uniform(subkeys[0], (SEQ_MIX, 1), minval=jnp.log(0.3), maxval=jnp.log(3.0)))
    base = jnp.clip(jax.random.normal(subkeys[1], (SEQ_MIX, HEADS * DV), jnp.float32), -2.0, 2.0)
    return (base * row_scale).astype(jnp.bfloat16)


def draw_token_rows(key, part):
    subkeys = jax.random.split(jax.random.fold_in(key, 23), 3)
    column_scale = jnp.exp(jax.random.uniform(subkeys[1], (1, D), minval=jnp.log(0.4), maxval=jnp.log(4.0)))
    row_scale = jnp.exp(jax.random.uniform(subkeys[0], (TOKENS_MOE, 1), minval=jnp.log(0.3), maxval=jnp.log(3.0)))
    base = jnp.clip(jax.random.normal(subkeys[2], (TOKENS_MOE, D), jnp.float32), -4.0, 4.0)
    return (base * row_scale * column_scale).astype(jnp.bfloat16)


def steps_of(stream_key, shape, cuts, smallest, top_value):
    loudness = 1.0
    for position, shards_of in cuts:
        heights = jax.random.uniform(jax.random.fold_in(jax.random.fold_in(stream_key, 6), position), (shards_of,), jnp.float32, smallest / len(cuts), top_value / len(cuts))
        loudness = loudness * jnp.repeat(jnp.exp(heights), shape[position] // shards_of).reshape((-1,) + (1,) * (len(shape) - 1 - position))
    return loudness


def shared_out(rng, own, number, rows, number_of, top, most, lean):
    sequence = jax.random.permutation(rng, number_of)
    packed, usual = load_shares(number_of, rows * top, most, lean, True), load_shares(number_of, rows * top, most, lean, False)
    places = jnp.arange(number_of)

    def named(sizes, rotation):
        used = int((sizes > 0).sum())
        fixed = max(1, used // 4)
        moved = fixed + (places - fixed + rotation * (used - fixed)) % max(1, number_of - fixed)
        return jnp.zeros((number_of,), jnp.int32).at[sequence[jnp.where(places < fixed, places, moved)]].set(jnp.asarray(sizes, jnp.int32))

    sizes = jnp.where(number % 4 == 0, named(packed, number // 4), named(usual, number - number // 4 - 1))
    mixed = jax.random.permutation(jax.random.fold_in(own, 3), number_of)
    donor, receiver = mixed[0:number_of // 2 * 2:2], mixed[1:number_of // 2 * 2:2]
    slack = jnp.minimum(sizes[donor] - 1, most - sizes[receiver]) // 2
    slack = jnp.where((donor == sequence[0]) | (receiver == sequence[0]) | (sizes[receiver] == 0), 0, jnp.maximum(slack, 0))
    moved = jax.random.randint(jax.random.fold_in(own, 4), (number_of // 2,), 0, 1 << 20) % (slack + 1)
    sizes = sizes.at[donor].add(-moved).at[receiver].add(moved)
    items = jnp.searchsorted(jnp.cumsum(sizes), jnp.arange(rows * top), side="right").astype(jnp.int32)
    table = items.reshape(top, rows).T
    table = table[jax.random.permutation(jax.random.fold_in(own, 1), rows)]
    rotation = jax.random.randint(jax.random.fold_in(own, 2), (rows, 1), 0, top)
    return jnp.take_along_axis(table, (jnp.arange(top)[None, :] + rotation) % top, axis=1)


def load_shares(count, total, most, slope, full):
    loads = [(1 << 20) // math.isqrt(grade ** slope) + 1 for grade in range(1, count + 1)]
    largest = most if full else min(most, max(-(-total // count), total * loads[0] // sum(loads)))
    least = 1 if total - largest >= count - 1 else 0
    counts, surplus = [largest] + [least] * (count - 1), total - largest - least * (count - 1)
    while surplus > 0:
        candidates = [i for i in range(1, count) if counts[i] < largest] or [i for i in range(1, count) if counts[i] < most]
        mass, budget = sum([loads[i] for i in candidates]), surplus
        for i in candidates:
            addition = min(most - counts[i], max(1, budget * loads[i] // mass), surplus)
            counts[i] = counts[i] + addition
            surplus = surplus - addition
    return np.array(counts)


def gaussian(own_key, dims, deviation, limit, cuts=(), held_as=jnp.bfloat16):
    factor_of = steps_of(own_key, dims, cuts, -0.22, 0.18) if cuts else 1.0
    entries = jax.random.normal(own_key, dims, jnp.float32) * deviation * factor_of
    return jnp.minimum(jnp.maximum(entries, -limit), limit).astype(held_as)


def setup_inputs(seed: int = 0) -> dict:
    keys = jax.random.split(jax.random.key(seed), 15)
    query_in = gaussian(keys[0], (SEQ_MIX, HEADS * DK), 1.0, 6.0, ((0, 8), (1, 4)))
    key_in = gaussian(keys[1], (SEQ_MIX, HEADS * DK), 1.0, 6.0, ((0, 8), (1, 4)))
    value_in = draw_value_in(jax.random.fold_in(keys[14], 71), 0)
    gate_in = gaussian(keys[3], (SEQ_MIX, HEADS * DV), 1.0, 6.0, ((0, 8), (1, 4)))
    decay_rate = draw_decay_rate(jax.random.fold_in(keys[14], 71), 0)
    head_gain = jnp.clip(1.0 + 0.18 * jax.random.normal(keys[5], (HEADS * DV,), jnp.float32), 0.1, 1.9)
    output_weight = gaussian(keys[6], (HEADS * DV, D), (HEADS * DV) ** -0.5, 0.125, ((0, 4),))
    token_rows = draw_token_rows(jax.random.fold_in(keys[14], 71), 0)
    token_gain = jnp.clip(1.0 + 0.18 * jax.random.normal(keys[8], (D,), jnp.float32), 0.1, 1.9)
    route_ids_keys = jax.random.split(jax.random.fold_in(keys[9], 1), TOKENS_MOE // TOK_MOE)
    route_ids_turns = jax.random.permutation(jax.random.fold_in(keys[9], 3), TOKENS_MOE // TOK_MOE)
    route_ids = jax.vmap(lambda own, number: shared_out(jax.random.fold_in(keys[9], 2), own, number, TOK_MOE, EXPERTS, TOP, CAP, 1))(route_ids_keys, route_ids_turns).reshape((TOKENS_MOE, TOP))
    route_weights = jnp.clip(jnp.exp(math.log(2.5) - 2.3025851 * jax.random.uniform(keys[10], (TOKENS_MOE, TOP), jnp.float32) ** steps_of(keys[10], (TOKENS_MOE, TOP), ((0, 8),), -0.2, 0.2)), 0.25, 2.5)
    expert_gate = gaussian(keys[11], (EXPERTS, D, FF), D ** -0.5, 0.125, ((0, 8), (2, 4)))
    expert_up = gaussian(keys[12], (EXPERTS, D, FF), D ** -0.5, 0.125, ((0, 8), (2, 4)))
    expert_down = gaussian(keys[13], (EXPERTS, FF, D), FF ** -0.5, 0.09375, ((0, 8), (2, 4)))
    return dict(query_in=query_in, key_in=key_in, value_in=value_in, gate_in=gate_in, decay_rate=decay_rate, head_gain=head_gain, output_weight=output_weight, token_rows=token_rows, token_gain=token_gain, route_ids=route_ids, route_weights=route_weights, expert_gate=expert_gate, expert_up=expert_up, expert_down=expert_down)


epsilon = 1e-06
rope_base = 10000.0

def rotate(values, positions):
    half_dim = values.shape[-1] // 2
    frequency = rope_base ** (-jnp.arange(half_dim, dtype=jnp.float32) * 2.0 / values.shape[-1])
    angles = positions.astype(jnp.float32)[:, None] * frequency[None, :]
    cosine_table = jnp.cos(angles)[:, None, :]
    sine_table = jnp.sin(angles)[:, None, :]
    first_half = values[..., :half_dim]
    second = values[..., half_dim:]
    return jnp.concatenate([first_half * cosine_table - second * sine_table, second * cosine_table + first_half * sine_table], -1)

def retention(query_in, key_in, value_in, gate_in, decay_rate, head_gain, output_weight):
    seq_length = query_in.shape[0]
    blocks = seq_length // TOK_MIX
    head_count = decay_rate.shape[0]
    highest = lax.Precision.HIGHEST
    positions = jnp.arange(seq_length, dtype=jnp.int32)
    rot_query = rotate(query_in.astype(jnp.float32).reshape(seq_length, head_count, DK), positions).astype(jnp.bfloat16)
    rot_key = (rotate(key_in.astype(jnp.float32).reshape(seq_length, head_count, DK), positions) * DK ** (-0.5)).astype(jnp.bfloat16)
    value_heads = value_in.reshape(seq_length, head_count, DV)
    within = jnp.arange(TOK_MIX, dtype=jnp.float32)
    distance = within[:, None] - within[None, :]
    decay_mat = jnp.where(distance[None] >= 0, jnp.exp(-decay_rate[:, None, None] * jnp.maximum(distance, 0.0)[None]), 0.0)
    key_decay = jnp.exp(-decay_rate[None, :] * (TOK_MIX - 1.0 - within)[:, None])
    query_decay = jnp.exp(-decay_rate[None, :] * (within + 1.0)[:, None])
    span_decay = jnp.exp(-decay_rate * TOK_MIX)

    def one_block(pieces):
        query_block, key_block, value_block = pieces
        scores = jnp.einsum('ihd,jhd->hij', query_block.astype(jnp.float32), key_block.astype(jnp.float32), precision=highest)
        weights = (scores * decay_mat).astype(jnp.bfloat16)
        local_out = jnp.einsum('hij,jhe->ihe', weights.astype(jnp.float32), value_block.astype(jnp.float32), precision=highest)
        decayed = (key_block.astype(jnp.float32) * key_decay[:, :, None]).astype(jnp.bfloat16)
        block_state = jnp.einsum('jhd,jhe->hde', decayed.astype(jnp.float32), value_block.astype(jnp.float32), precision=highest)
        return (local_out, block_state)
    query_blocks = rot_query.reshape(blocks, TOK_MIX, head_count, DK)
    local_out, states = lax.map(one_block, (query_blocks, rot_key.reshape(blocks, TOK_MIX, head_count, DK), value_heads.reshape(blocks, TOK_MIX, head_count, DV)))

    def carry_step(running, block_state):
        return (running * span_decay[:, None, None] + block_state, running)
    initial = jnp.zeros((head_count, DK, DV), jnp.float32)
    final_state, carried = lax.scan(carry_step, initial, states)
    carried_out = jnp.einsum('bihd,bhde->bihe', query_blocks.astype(jnp.float32), carried, precision=highest) * query_decay[None, :, :, None]
    retained = (local_out + carried_out).reshape(seq_length, head_count, DV)
    centered = retained - lax.optimization_barrier(jnp.mean(retained, -1, keepdims=True))
    normed = centered * lax.rsqrt(lax.optimization_barrier(jnp.mean(centered * centered, -1, keepdims=True)) + epsilon)
    mixed = (normed.reshape(seq_length, head_count * DV) * head_gain * jax.nn.silu(gate_in.astype(jnp.float32))).astype(jnp.bfloat16)
    group_width = head_count // N_TP * DV

    def add_group(group_index, summed):
        first_col = (group_index * group_width).astype(jnp.int32)
        columns = lax.dynamic_slice_in_dim(mixed, first_col, group_width, 1)
        weight_rows = lax.dynamic_slice_in_dim(output_weight, first_col, group_width, 0)
        group_part = jnp.dot(columns, weight_rows, preferred_element_type=jnp.float32).astype(jnp.bfloat16)
        return summed + lax.optimization_barrier(group_part).astype(jnp.float32)
    summed = lax.fori_loop(0, N_TP, add_group, jnp.zeros((seq_length, output_weight.shape[1]), jnp.float32))
    return summed.astype(jnp.bfloat16)

def experts(token_rows, token_gain, route_ids, route_weights, expert_gate, expert_up, expert_down):
    token_count, model_dim = token_rows.shape
    rows_float = token_rows.astype(jnp.float32)
    normed = (rows_float * lax.rsqrt(lax.optimization_barrier(jnp.mean(rows_float * rows_float, -1, keepdims=True)) + epsilon) * token_gain).astype(jnp.bfloat16)
    padded = jnp.concatenate([normed, jnp.zeros((1, model_dim), jnp.bfloat16)], 0)
    expert_count = expert_gate.shape[0]
    flat_ids = route_ids.reshape(-1)
    pair_count = flat_ids.shape[0]
    per_block = TOK_MOE * TOP
    matches = (flat_ids[:, None] == jnp.arange(expert_count, dtype=jnp.int32)[None, :]).astype(jnp.int32)
    running = jnp.cumsum(matches.reshape(N_EP, per_block, expert_count), axis=1).reshape(pair_count, expert_count)
    slot_number = lax.optimization_barrier(jnp.sum((running - 1) * matches, axis=1)).astype(jnp.int32)
    source = (jnp.arange(pair_count, dtype=jnp.int32) // per_block).astype(jnp.int32)
    slot_index = (flat_ids * (N_EP * CAP) + source * CAP + slot_number).astype(jnp.int32)
    token_index = (jnp.arange(pair_count, dtype=jnp.int32) // TOP).astype(jnp.int32)
    slot_table = jnp.full((expert_count * N_EP * CAP,), token_count, jnp.int32).at[slot_index].set(token_index)

    def one_expert(pieces):
        table_rows, gate_weight, up_weight, down_weight = pieces
        inputs = padded[table_rows]
        gate_pre = jnp.dot(inputs, gate_weight, preferred_element_type=jnp.float32)
        up_pre = jnp.dot(inputs, up_weight, preferred_element_type=jnp.float32)
        hidden = (jax.nn.silu(gate_pre) * up_pre).astype(jnp.bfloat16)
        return jnp.dot(hidden, down_weight, preferred_element_type=jnp.float32).astype(jnp.bfloat16)
    results = lax.map(one_expert, (slot_table.reshape(expert_count, N_EP * CAP), expert_gate, expert_up, expert_down))
    picked = results.reshape(-1, model_dim)[slot_index].astype(jnp.float32).reshape(token_count, TOP, model_dim)
    combined = lax.optimization_barrier(jnp.sum(picked * route_weights[:, :, None], axis=1))
    return combined.astype(jnp.bfloat16)

def reference(query_in, key_in, value_in, gate_in, decay_rate, head_gain, output_weight, token_rows, token_gain, route_ids, route_weights, expert_gate, expert_up, expert_down):
    retained_out = retention(query_in, key_in, value_in, gate_in, decay_rate, head_gain, output_weight)
    expert_out = experts(token_rows, token_gain, route_ids, route_weights, expert_gate, expert_up, expert_down)
    return (retained_out, expert_out)
```

```python
import functools

import jax
import jax.numpy as jnp
from jax import lax
from jax.experimental import pallas as pl
from jax.experimental.pallas import tpu as pltpu
from jax.sharding import PartitionSpec as P

epsilon = 1e-06
rope_base = 10000.0
F32 = jnp.float32
BF16 = jnp.bfloat16
MESH = pl.DeviceIdType.MESH


def dot(a, b):
    return jnp.dot(a, b, preferred_element_type=F32)


def iota(shape, dim):
    return lax.broadcasted_iota(jnp.int32, shape, dim)


def silu(v):
    return v / (1.0 + jnp.exp(-v))


def kernel(
    size,
    tok, tgain, ids, ids_t, rweights, decay, hgain, cos_t, sin_t,
    query_h, key_h, value_h, gate_h, ow_h, wg_h, wu_h, wd_h,
    ret_out, exp_out,
    query, key, value, gate, ow, wg, wu, wd,
    obuf, xbuf, hbuf, sbuf, rbuf, w_hi, w_lo,
    rq, rk, local, state, st_send, st_recv, mixed, part, rs1, rs2_send, rs2_recv,
    load_sem, d_send, d_recv, xy_send, xy_recv, xc_send, xc_recv,
    hy_send, hy_recv, hc_send, hc_recv, b_send, b_recv, st_ssem, st_rsem,
    r1_send, r1_recv, r2_send, r2_recv,
):
    ep, tp, cap, fan, rounds, nf, nm = (
        size["ep"], size["tp"], size["cap"], size["fan"], size["rounds"], size["nf"], size["nm"]
    )
    ys = tp // 2
    e, t = lax.axis_index("ep"), lax.axis_index("tp")
    y, c = t // 2, lax.rem(t, 2)
    mate = (e, y * 2 + 1 - c)
    heads = decay.shape[0]
    tokens, model = tok.shape
    cw = model // tp
    block_len = query.shape[0]
    dk = query.shape[1] // heads

    def over_ep(offset):
        return (lax.rem(e + offset, ep), t)

    def y_at(offset):
        return lax.rem(y + offset, ys)

    def over_y(offset):
        return (e, y_at(offset) * 2 + c)

    def remote(src, dst, ssem, rsem, device):
        return pltpu.make_async_remote_copy(
            src_ref=src, dst_ref=dst, send_sem=ssem, recv_sem=rsem,
            device_id=device, device_id_type=MESH,
        )

    sent = []

    def send(src, dst, ssem, rsem, device):
        copy = remote(src, dst, ssem, rsem, device)
        copy.start()
        sent.append(copy)

    def arrived(dst, ssem, rsem, device):
        remote(dst, dst, ssem, rsem, device).wait_recv()

    loads = [
        pltpu.make_async_copy(a, b, load_sem.at[i])
        for i, (a, b) in enumerate(
            ((query_h, query), (key_h, key), (value_h, value), (gate_h, gate),
             (wg_h, wg), (wu_h, wu), (ow_h, ow), (wd_h, wd))
        )
    ]
    for copy in loads:
        copy.start()

    barrier = pltpu.get_barrier_semaphore()
    friends = [over_ep(i) for i in range(1, ep)] + [over_y(i) for i in range(1, ys)] + [mate]
    for friend in friends:
        pl.semaphore_signal(barrier, inc=1, device_id=friend, device_id_type=MESH)

    def relative(v):
        return jnp.where(v < e, v - e + ep, v - e)

    rel = relative(ids[...])
    rel_t = relative(ids_t[...])
    lanes = max(ep, 128)
    named0 = iota((tokens, lanes), 1) == rel[:, 0:1]
    named1 = iota((tokens, lanes), 1) == rel[:, 1:2]
    named = jnp.where(named0 | named1, 1.0, 0.0)
    before = jnp.where(iota((tokens, tokens), 1) < iota((tokens, tokens), 0), 1.0, 0.0)
    rank = dot(before.astype(BF16), named.astype(BF16))
    pos0 = rel[:, 0:1] * cap + jnp.sum(
        jnp.where(named0, rank, 0.0), 1, keepdims=True).astype(jnp.int32)
    pos1 = rel[:, 1:2] * cap + jnp.sum(
        jnp.where(named1, rank, 0.0), 1, keepdims=True).astype(jnp.int32)
    rows = max(ep, 16)
    named0_t = iota((rows, tokens), 0) == rel_t[0:1, :]
    named1_t = iota((rows, tokens), 0) == rel_t[1:2, :]
    named_t = jnp.where(named0_t | named1_t, 1.0, 0.0)
    after = jnp.where(iota((tokens, tokens), 0) < iota((tokens, tokens), 1), 1.0, 0.0)
    rank_t = dot(named_t.astype(BF16), after.astype(BF16))
    pos0_t = rel_t[0:1, :] * cap + jnp.sum(
        jnp.where(named0_t, rank_t, 0.0), 0, keepdims=True).astype(jnp.int32)
    pos1_t = rel_t[1:2, :] * cap + jnp.sum(
        jnp.where(named1_t, rank_t, 0.0), 0, keepdims=True).astype(jnp.int32)

    rows_float = tok[...].astype(F32)
    scale = lax.rsqrt(jnp.mean(rows_float * rows_float, -1, keepdims=True) + epsilon)
    own = pl.ds(pl.multiple_of(t * cw, cw), cw)
    normed = (tok[:, own].astype(F32) * scale * tgain[:, own]).astype(BF16)
    row_id = iota((ep * cap, tokens), 0)
    pick = jnp.where((row_id == pos0_t) | (row_id == pos1_t), 1.0, 0.0).astype(BF16)
    obuf[...] = dot(pick, normed).astype(BF16)

    pl.semaphore_wait(barrier, len(friends))

    def block(j, n=1):
        return pl.ds(j * cap, n * cap)

    for j in range(ep - 1, 0, -1):
        back = ep - j
        send(obuf.at[block(j)], xbuf.at[t, block(back)], d_send.at[j], d_recv.at[back], over_ep(j))
    xbuf[t, block(0), :] = obuf[block(0), :]

    for copy in loads[:3]:
        copy.wait()
    within = iota((block_len, 1), 0).astype(F32)

    def head_cols(h):
        return pl.ds(pl.multiple_of(h * dk, dk), dk)

    def turn(x):
        return x * cos_t[...] + pltpu.roll(x, dk // 2, 1) * sin_t[...]

    def head_state(h, carry):
        cols = head_cols(h)
        rate = decay[h]
        rq[:, cols] = turn(query[:, cols].astype(F32)).astype(BF16)
        rot_key = (turn(key[:, cols].astype(F32)) * dk ** (-0.5)).astype(BF16)
        rk[:, cols] = rot_key
        decayed = (rot_key.astype(F32) * jnp.exp(-rate * (block_len - 1.0 - within))).astype(BF16)
        now = lax.dot_general(
            decayed, value[:, cols], (((0,), (0,)), ((), ())), preferred_element_type=F32)
        st_send[0, h] = now.astype(BF16)
        return carry

    lax.fori_loop(0, heads, head_state, 0)
    for i in range(1, fan + 1):
        send(st_send.at[0], st_recv.at[i - 1], st_ssem.at[i - 1], st_rsem.at[i - 1], over_ep(i))

    col = iota((tokens, ep * cap), 1)
    weight = jnp.where(col == pos0, rweights[:, 0:1], 0.0) + jnp.where(
        col == pos1, rweights[:, 1:2], 0.0)
    high = weight.astype(BF16)
    w_hi[...] = high
    w_lo[...] = (weight - high.astype(F32)).astype(BF16)

    chunk = min(128, block_len)

    def head_local(h):
        cols = head_cols(h)
        rate = decay[h]
        key_grow = jnp.exp(rate * iota((1, block_len), 1).astype(F32))

        def step(i, carry):
            rws = pl.ds(pl.multiple_of(i * chunk, chunk), chunk)
            place = i * chunk + iota((chunk, 1), 0)
            scores = lax.dot_general(
                rq[rws, cols], rk[:, cols], (((1,), (1,)), ((), ())), preferred_element_type=F32)
            fade = jnp.exp(-rate * place.astype(F32)) * key_grow
            seen = iota((chunk, block_len), 1) <= place
            weights = jnp.where(seen, scores * fade, 0.0).astype(BF16)
            local[rws, cols] = dot(weights, value[:, cols])
            return carry

        lax.fori_loop(0, block_len // chunk, step, 0)

    def spread(buf, piece, rws, ysend, yrecv, csend, crecv, g):
        for a in range(1, ys):
            send(buf.at[piece, rws], buf.at[piece, rws], ysend.at[a, g], yrecv.at[a, g], over_y(a))
        send(buf.at[piece, rws], buf.at[piece, rws], csend.at[0, g], crecv.at[0, g], mate)

    def pass_on(buf, rws, ysend, yrecv, csend, crecv, g):
        for a in range(1, ys):
            piece = y_at(ys - a) * 2 + c
            arrived(buf.at[piece, rws], ysend.at[a, g], yrecv.at[a, g], over_y(a))
            send(buf.at[piece, rws], buf.at[piece, rws], csend.at[a, g], crecv.at[a, g], mate)

    def collect(buf, rws, csend, crecv, g):
        for a in range(ys):
            piece = y_at(ys - a) * 2 + 1 - c
            arrived(buf.at[piece, rws], csend.at[a, g], crecv.at[a, g], mate)

    per_f = ep // nf
    done = 0
    for f in range(nf):
        for k in range(f * per_f, (f + 1) * per_f):
            if k > 0:
                arrived(xbuf.at[t, block(k)], d_send.at[k], d_recv.at[k], over_ep(k))
        spread(xbuf, t, block(f * per_f, per_f), xy_send, xy_recv, xc_send, xc_recv, f)
        if f > 0:
            pass_on(xbuf, block((f - 1) * per_f, per_f), xy_send, xy_recv, xc_send, xc_recv, f - 1)
        upto = heads * (f + 1) // nf
        for h in range(done, upto):
            head_local(h)
        done = upto
    last = nf - 1
    f_per_m = nf // nm
    per_m = ep // nm
    ff = wg.shape[1]
    n_tile = min(256, ff)
    loads[4].wait()
    loads[5].wait()

    def lane(h, times):
        return jnp.exp(jnp.full((1, dk), -decay[h] * (block_len * times), F32))

    def first_state():
        for i in range(fan):
            arrived(st_recv.at[i], st_ssem.at[i], st_rsem.at[i], over_ep(i + 1))

        def one(h, carry):
            total = jnp.zeros((dk, dk), F32)
            for i in range(fan):
                took = st_recv[i, h].astype(F32) * lane(h, float(i))
                total += jnp.where(e > i, took, 0.0)
            state[h] = total
            return carry

        lax.fori_loop(0, heads, one, 0)

    def state_send(r):
        def one(h, carry):
            st_send[r + 1, h] = state[h].astype(BF16)
            return carry

        lax.fori_loop(0, heads, one, 0)
        send(st_send.at[r + 1], st_recv.at[fan + r], st_ssem.at[fan + r], st_rsem.at[fan + r],
             over_ep(fan * 2**r))

    def state_take(r):
        offset = fan * 2**r
        arrived(st_recv.at[fan + r], st_ssem.at[fan + r], st_rsem.at[fan + r], over_ep(offset))

        def one(h, carry):
            took = st_recv[fan + r, h].astype(F32) * lane(h, float(offset))
            state[h] = state[h] + jnp.where(e >= offset, took, 0.0)
            return carry

        lax.fori_loop(0, heads, one, 0)

    for m in range(nm):
        for f in range(m * f_per_m, (m + 1) * f_per_m):
            if f == last:
                pass_on(xbuf, block(f * per_f, per_f), xy_send, xy_recv, xc_send, xc_recv, f)
            collect(xbuf, block(f * per_f, per_f), xc_send, xc_recv, f)
        rws = block(m * per_m, per_m)

        def tile(n, carry):
            cols = pl.ds(pl.multiple_of(n * n_tile, n_tile), n_tile)
            g = u = None
            for p in range(tp):
                x = xbuf[p, rws, :]
                ins = pl.ds(p * cw, cw)
                gp, up = dot(x, wg[ins, cols]), dot(x, wu[ins, cols])
                g, u = (gp, up) if g is None else (g + gp, u + up)
            hbuf[t, rws, cols] = (silu(g) * u).astype(BF16)
            return carry

        lax.fori_loop(0, ff // n_tile, tile, 0)
        spread(hbuf, t, rws, hy_send, hy_recv, hc_send, hc_recv, m)
        if m == 0:
            first_state()
            if rounds:
                state_send(0)
    for r in range(rounds):
        if r > 0:
            state_send(r)
        state_take(r)

    loads[3].wait()
    loads[6].wait()

    def finish(n, carry):
        h, i = n // (block_len // chunk), lax.rem(n, block_len // chunk)
        cols = head_cols(h)
        rws = pl.ds(pl.multiple_of(i * chunk, chunk), chunk)
        place = (i * chunk + iota((chunk, 1), 0)).astype(F32)
        held = state[h]
        high = held.astype(BF16)
        low = (held - high.astype(F32)).astype(BF16)
        q = rq[rws, cols]
        retained = local[rws, cols] + (dot(q, high) + dot(q, low)) * jnp.exp(
            -decay[h] * (place + 1.0))
        centered = retained - jnp.mean(retained, -1, keepdims=True)
        out = centered * lax.rsqrt(jnp.mean(centered * centered, -1, keepdims=True) + epsilon)
        mixed[rws, cols] = (out * hgain[:, cols] * silu(gate[rws, cols].astype(F32))).astype(BF16)
        return carry

    lax.fori_loop(0, heads * (block_len // chunk), finish, 0)
    rb = block_len // tp
    o_tile = min(512, model)

    def project(n, carry):
        cols = pl.ds(pl.multiple_of(n * o_tile, o_tile), o_tile)
        for d in range(tp):
            part[d, :, cols] = dot(mixed[pl.ds(d * rb, rb), :], ow[:, cols]).astype(BF16)
        return carry

    lax.fori_loop(0, model // o_tile, project, 0)
    for b in range(ys):
        send(part.at[b * 2 + 1 - c], rs1.at[b], r1_send.at[b], r1_recv.at[b], mate)

    def h_pass(m):
        pass_on(hbuf, block(m * per_m, per_m), hy_send, hy_recv, hc_send, hc_recv, m)

    def sum_over_cores():
        for b in range(ys):
            arrived(rs1.at[b], r1_send.at[b], r1_recv.at[b], mate)
        for a in range(1, ys):
            b = y_at(a)
            rs2_send[a - 1] = (part[b * 2 + c].astype(F32) + rs1[b].astype(F32)).astype(BF16)
            send(rs2_send.at[a - 1], rs2_recv.at[a - 1], r2_send.at[a - 1], r2_recv.at[a - 1],
                 over_y(a))

    d_tile = min(256, cw)
    loads[7].wait()
    for m in range(nm):
        h_pass(m)
        if m == 0:
            sum_over_cores()
        rws = block(m * per_m, per_m)
        collect(hbuf, rws, hc_send, hc_recv, m)

        def down(n, carry):
            cols = pl.ds(pl.multiple_of(n * d_tile, d_tile), d_tile)
            total = None
            for p in range(tp):
                now = dot(hbuf[p, rws, :], wd[pl.ds(p * ff, ff), cols])
                total = now if total is None else total + now
            sbuf[rws, cols] = total.astype(BF16)
            return carry

        lax.fori_loop(0, cw // d_tile, down, 0)
        for k in range(m * per_m, (m + 1) * per_m):
            if k > 0:
                back = ep - k
                send(sbuf.at[block(k)], rbuf.at[block(back)], b_send.at[k], b_recv.at[back],
                     over_ep(k))
            else:
                rbuf[block(0), :] = sbuf[block(0), :]

    total = part[t].astype(F32) + rs1[y].astype(F32)
    for a in range(1, ys):
        arrived(rs2_recv.at[a - 1], r2_send.at[a - 1], r2_recv.at[a - 1], over_y(a))
        total += rs2_recv[a - 1].astype(F32)
    ret_out[...] = total.astype(BF16)
    for k in range(1, ep):
        arrived(rbuf.at[block(k)], b_send.at[k], b_recv.at[k], over_ep(k))
    exp_out[...] = (dot(w_hi[...], rbuf[...]) + dot(w_lo[...], rbuf[...])).astype(BF16)
    for copy in sent:
        copy.wait_send()


def body(
    query_in, key_in, value_in, gate_in, decay_rate, head_gain, output_weight,
    token_rows, token_gain, route_ids, route_weights, expert_gate, expert_up, expert_down,
):
    ep, tp = lax.axis_size("ep"), lax.axis_size("tp")
    tokens, model = token_rows.shape
    top = route_ids.shape[1]
    cap = -(-(2 * tokens * top // ep) // 32) * 32
    block_len, width = query_in.shape
    heads = decay_rate.shape[0]
    dk = width // heads
    ff = expert_gate.shape[2]
    cw = expert_down.shape[2]
    ys = tp // 2
    fan = min(4, ep - 1)
    rounds = 0
    while fan * 2**rounds < ep - 1:
        rounds += 1
    nf, nm = 4, 2
    half = dk // 2
    positions = lax.axis_index("ep") * block_len + jnp.arange(block_len, dtype=jnp.int32)
    frequency = rope_base ** (-jnp.arange(half, dtype=F32) * 2.0 / dk)
    angles = positions.astype(F32)[:, None] * frequency[None, :]
    cosine, sine = jnp.cos(angles), jnp.sin(angles)
    cos_t = jnp.concatenate([cosine, cosine], -1)
    sin_t = jnp.concatenate([-sine, sine], -1)
    size = dict(ep=ep, tp=tp, cap=cap, fan=fan, rounds=rounds, nf=nf, nm=nm)
    slots = ep * cap
    rb = block_len // tp
    vmem = pl.BlockSpec(memory_space=pltpu.VMEM)
    smem = pl.BlockSpec(memory_space=pltpu.SMEM)
    hbm = pl.BlockSpec(memory_space=pl.ANY)
    dma = pltpu.SemaphoreType.DMA
    big = [query_in, key_in, value_in, gate_in, output_weight,
           expert_gate[0], expert_up[0], expert_down[0]]
    held = big
    return pl.pallas_call(
        functools.partial(kernel, size),
        out_shape=(
            jax.ShapeDtypeStruct((rb, model), BF16),
            jax.ShapeDtypeStruct((tokens, cw), BF16),
        ),
        in_specs=[vmem] * 5 + [smem] + [vmem] * 3 + [hbm] * 8,
        out_specs=(vmem, vmem),
        scratch_shapes=[pltpu.VMEM(a.shape, BF16) for a in held]
        + [
            pltpu.VMEM((slots, cw), BF16),
            pltpu.VMEM((tp, slots, cw), BF16),
            pltpu.VMEM((tp, slots, ff), BF16),
            pltpu.VMEM((slots, cw), BF16),
            pltpu.VMEM((slots, cw), BF16),
            pltpu.VMEM((tokens, slots), BF16),
            pltpu.VMEM((tokens, slots), BF16),
            pltpu.VMEM((block_len, width), BF16),
            pltpu.VMEM((block_len, width), BF16),
            pltpu.VMEM((block_len, width), F32),
            pltpu.VMEM((heads, dk, dk), F32),
            pltpu.VMEM((1 + rounds, heads, dk, dk), BF16),
            pltpu.VMEM((fan + rounds, heads, dk, dk), BF16),
            pltpu.VMEM((block_len, width), BF16),
            pltpu.VMEM((tp, rb, model), BF16),
            pltpu.VMEM((ys, rb, model), BF16),
            pltpu.VMEM((max(ys - 1, 1), rb, model), BF16),
            pltpu.VMEM((max(ys - 1, 1), rb, model), BF16),
            dma((8,)),
            dma((ep,)), dma((ep,)),
            dma((ys, nf)), dma((ys, nf)), dma((ys, nf)), dma((ys, nf)),
            dma((ys, nm)), dma((ys, nm)), dma((ys, nm)), dma((ys, nm)),
            dma((ep,)), dma((ep,)),
            dma((fan + rounds,)), dma((fan + rounds,)),
            dma((ys,)), dma((ys,)), dma((ys,)), dma((ys,)),
        ],
        compiler_params=pltpu.CompilerParams(
            collective_id=0, has_side_effects=True, vmem_limit_bytes=60 * 2**20
        ),
    )(
        token_rows, token_gain[None, :], route_ids, route_ids.T, route_weights,
        decay_rate, head_gain[None, :], cos_t, sin_t,
        *big,
    )


def solution(mesh):
    placed = (
        P("ep", "tp"), P("ep", "tp"), P("ep", "tp"), P("ep", "tp"),
        P("tp"), P("tp"), P("tp", None), P("ep", None), P(),
        P("ep", None), P("ep", None),
        P("ep", None, "tp"), P("ep", None, "tp"), P("ep", None, "tp"),
    )
    return jax.shard_map(
        body,
        mesh=mesh,
        in_specs=placed,
        out_specs=(P(("ep", "tp"), None), P("ep", "tp")),
        check_vma=False,
    )
```
